32 devices in a mesh: sp: 8 (over z, x), tp: 4 (over y, core).
Axes of the slice: x: 2, y: 2, z: 4, core: 2. Of those that a mesh axis runs over, the one named last changes fastest.
Arguments:
- resid: bfloat16 [4096, 2048], P(('sp', 'tp')), may hold values from -6 to 6
- pool_in: bfloat16 [4096, 1024], P('sp', 'tp'), may hold values from -8 to 8
- doc_ids: int32 [4096], P('sp'), may hold values from 0 to 3, never falling along the last dimension, each value on 1 to 1536 neighbouring positions
- w_group: bfloat16 [8, 128, 128], replicated, may hold values from -0.5 to 0.5
- pool_scale: bfloat16 [1024], replicated, may hold values from 0.099609375 to 1.8984375
- w_branch: bfloat16 [1024, 2048], P('tp'), may hold values from -0.1875 to 0.1875
- norm_gain: bfloat16 [2048], replicated, may hold values from 0.099609375 to 1.8984375
- route_ids: int32 [4096, 4], P(('sp', 'tp')), may hold values from 0 to 31, all different within a row; in each aligned block of 128 rows (0 to 127, 128 to 255, ...) at most 32 rows name the same one
- route_wts: float32 [4096, 4], P(('sp', 'tp')), may hold values from 0.2 to 1
- w_exp_gate: bfloat16 [32, 2048, 512], P(('sp', 'tp')), may hold values from -0.125 to 0.125
- w_exp_up: bfloat16 [32, 2048, 512], P(('sp', 'tp')), may hold values from -0.125 to 0.125
- w_exp_down: bfloat16 [32, 512, 2048], P(('sp', 'tp')), may hold values from -0.25 to 0.25
- w_sh_gate: bfloat16 [2048, 512], replicated, may hold values from -0.125 to 0.125
- w_sh_up: bfloat16 [2048, 512], replicated, may hold values from -0.125 to 0.125
- w_sh_down: bfloat16 [512, 2048], replicated, may hold values from -0.25 to 0.25
- final_gain: bfloat16 [2048], replicated, may hold values from 0.099609375 to 1.8984375
Outputs:
- final: bfloat16 [4096, 2048], P(('sp', 'tp'))
The draws below stay inside these ranges and needn't reach their ends.
Inputs may be any that keep to these rules, and one draw needn't show every extreme that they name: `doc_ids`: never falls along the positions. `route_ids`: each row names 4 different experts; among the rows of one device (aligned blocks of 128 rows) no expert is named by more than 32 rows, a bound that some block reaches.
All inputs are finite; a program needn't handle non-finite values.
Results may differ from the reference program's by a relative error of at most 0.0062.
Values may be sent and summed in bfloat16 or wider, within the bound.
No kernel may reach another device: no remote copies, remote signals or barrier semaphores. Data moves between devices by JAX's collectives and lax.ppermute only.
A program may use at most 128 MiB of HBM per device.

```python
import math
import jax
import jax.numpy as jnp
import numpy as np
from jax import lax

D = 2048
GROUP_CH = 128
GROUPS = 8
FF = 512
TOPK = 4
ROWS = 128
P_SIZE = 1024
EXPERTS = 32
TOK_DEV = 512
TOKENS = 4096
CAP = 32
N_SP = 8
DEVICES = 32


def draw_pool_in(key, part):
    offset_key = jax.random.fold_in(key, 11)
    noise_key = jax.random.fold_in(key, 12)
    block_count = TOKENS // 64
    offsets = jnp.clip(jax.random.normal(offset_key, (block_count, P_SIZE), jnp.float32) * 1.5, -4.0, 4.0)
    cell_noise = jnp.clip(jax.random.normal(noise_key, (TOKENS, P_SIZE), jnp.float32), -4.0, 4.0)
    return (jnp.repeat(offsets, 64, axis=0) + cell_noise).astype(jnp.bfloat16)


def block_scale(rng, dims, pieces, least, largest):
    loudness = 1.0
    for axis_at, shards_of in pieces:
        steps = jax.random.uniform(jax.random.fold_in(jax.random.fold_in(rng, 6), axis_at), (shards_of,), jnp.float32, least / len(pieces), largest / len(pieces))
        loudness = loudness * jnp.repeat(jnp.exp(steps), dims[axis_at] // shards_of).reshape((-1,) + (1,) * (len(dims) - 1 - axis_at))
    return loudness


def profile(count, total, bound, skew):
    portions = [(1 << 20) // math.isqrt(standing ** skew) + 1 for standing in range(2, count + 1)]
    rest, given = total - bound - (count - 1), [1] * (count - 1)
    while rest > 0:
        free = [i for i in range(count - 1) if given[i] < bound]
        mass, budget = sum([portions[i] for i in free]), rest
        for i in free:
            more = min(bound - given[i], max(1, budget * portions[i] // mass), rest)
            given[i] = given[i] + more
            rest = rest - more
    return np.array([bound] + given)


def uneven_parts(stream_key, amount, total, reach, lean):
    if amount == 2:
        one = jax.random.randint(stream_key, (), max(1, total - reach), min(reach, total - 1) + 1)
        return jnp.stack([one, total - one])
    sizes = jnp.asarray(profile(amount, total, reach, lean), jnp.int32)
    pairs = (amount - 1) // 2
    donor, receiver = sizes[1:1 + 2 * pairs:2], sizes[2:2 + 2 * pairs:2]
    slack = jnp.minimum(donor - 1, reach - receiver)
    passed = jax.random.randint(jax.random.fold_in(stream_key, 1), (pairs,), 0, 1 << 20) % (slack + 1)
    sizes = sizes.at[1:1 + 2 * pairs:2].set(donor - passed).at[2:2 + 2 * pairs:2].set(receiver + passed)
    return sizes[jax.random.permutation(jax.random.fold_in(stream_key, 2), amount)]


def assign_block(key, own, number, rows, number_of, top, reach, slope):
    sequence = jax.random.permutation(key, number_of)
    packed, common = portions_of(number_of, rows * top, reach, slope, True), portions_of(number_of, rows * top, reach, slope, False)
    places = jnp.arange(number_of)

    def named(sizes, offset_by):
        used = int((sizes > 0).sum())
        fixed = max(1, used // 4)
        passed = fixed + (places - fixed + offset_by * (used - fixed)) % max(1, number_of - fixed)
        return jnp.zeros((number_of,), jnp.int32).at[sequence[jnp.where(places < fixed, places, passed)]].set(jnp.asarray(sizes, jnp.int32))

    sizes = jnp.where(number % 4 == 0, named(packed, number // 4), named(common, number - number // 4 - 1))
    mixed = jax.random.permutation(jax.random.fold_in(own, 3), number_of)
    source_of, taker = mixed[0:number_of // 2 * 2:2], mixed[1:number_of // 2 * 2:2]
    slack = jnp.minimum(sizes[source_of] - 1, reach - sizes[taker]) // 2
    slack = jnp.where((source_of == sequence[0]) | (taker == sequence[0]) | (sizes[taker] == 0), 0, jnp.maximum(slack, 0))
    passed = jax.random.randint(jax.random.fold_in(own, 4), (number_of // 2,), 0, 1 << 20) % (slack + 1)
    sizes = sizes.at[source_of].add(-passed).at[taker].add(passed)
    labels = jnp.searchsorted(jnp.cumsum(sizes), jnp.arange(rows * top), side="right").astype(jnp.int32)
    grid = labels.reshape(top, rows).T
    grid = grid[jax.random.permutation(jax.random.fold_in(own, 1), rows)]
    offset_by = jax.random.randint(jax.random.fold_in(own, 2), (rows, 1), 0, top)
    return jnp.take_along_axis(grid, (jnp.arange(top)[None, :] + offset_by) % top, axis=1)


def portions_of(amount, total, limit, lean, full):
    portions = [(1 << 20) // math.isqrt(standing ** lean) + 1 for standing in range(1, amount + 1)]
    largest = limit if full else min(limit, max(-(-total // amount), total * portions[0] // sum(portions)))
    least = 1 if total - largest >= amount - 1 else 0
    holding, spare = [largest] + [least] * (amount - 1), total - largest - least * (amount - 1)
    while spare > 0:
        free = [i for i in range(1, amount) if holding[i] < largest] or [i for i in range(1, amount) if holding[i] < limit]
        mass, left = sum([portions[i] for i in free]), spare
        for i in free:
            extra = min(limit - holding[i], max(1, left * portions[i] // mass), spare)
            holding[i] = holding[i] + extra
            spare = spare - extra
    return np.array(holding)


def noise(rng, extent, width, bound, shards=(), kind=jnp.bfloat16):
    result = width * jax.random.normal(rng, extent, jnp.float32)
    if shards:
        result = result * block_scale(rng, extent, shards, -0.22, 0.18)
    return jnp.clip(result, -bound, bound).astype(kind)


def setup_inputs(seed: int = 0) -> dict:
    arg_keys = jax.random.split(jax.random.key(seed), 17)
    resid = noise(arg_keys[0], (TOKENS, D), 1.0, 6.0, ((0, 32),))
    pool_in = draw_pool_in(jax.random.fold_in(arg_keys[16], 71), 0)
    doc_ids = jnp.searchsorted(jnp.cumsum(uneven_parts(arg_keys[2], N_SP // 2, TOKENS, 3 * TOK_DEV, 1)), jnp.arange(TOKENS), side="right").astype(jnp.int32)
    w_group = noise(arg_keys[3], (GROUPS, GROUP_CH, GROUP_CH), GROUP_CH ** -0.5, 0.5)
    pool_scale = jnp.clip(1.0 + 0.18 * jax.random.normal(arg_keys[4], (P_SIZE,), jnp.float32), 0.099609375, 1.8984375).astype(jnp.bfloat16)
    w_branch = noise(arg_keys[5], (P_SIZE, D), P_SIZE ** -0.5, 0.1875, ((0, 4),))
    norm_gain = jnp.clip(1.0 + 0.18 * jax.random.normal(arg_keys[6], (D,), jnp.float32), 0.099609375, 1.8984375).astype(jnp.bfloat16)
    route_ids_keys = jax.random.split(jax.random.fold_in(arg_keys[7], 1), TOKENS // ROWS)
    route_ids_turns = jax.random.permutation(jax.random.fold_in(arg_keys[7], 3), TOKENS // ROWS)
    route_ids = jax.vmap(lambda own, number: assign_block(jax.random.fold_in(arg_keys[7], 2), own, number, ROWS, EXPERTS, TOPK, CAP, 2))(route_ids_keys, route_ids_turns).reshape((TOKENS, TOPK))
    route_wts = jnp.clip(0.2 + 0.8 * jax.random.uniform(arg_keys[8], (TOKENS, TOPK), jnp.float32) ** block_scale(arg_keys[8], (TOKENS, TOPK), ((0, 32),), -0.2, 0.2), 0.2, 1.0)
    w_exp_gate = noise(arg_keys[9], (EXPERTS, D, FF), D ** -0.5, 0.125, ((0, 32),))
    w_exp_up = noise(arg_keys[10], (EXPERTS, D, FF), D ** -0.5, 0.125, ((0, 32),))
    w_exp_down = noise(arg_keys[11], (EXPERTS, FF, D), FF ** -0.5, 0.25, ((0, 32),))
    w_sh_gate = noise(arg_keys[12], (D, FF), D ** -0.5, 0.125)
    w_sh_up = noise(arg_keys[13], (D, FF), D ** -0.5, 0.125)
    w_sh_down = noise(arg_keys[14], (FF, D), FF ** -0.5, 0.25)
    final_gain = jnp.clip(1.0 + 0.18 * jax.random.normal(arg_keys[15], (D,), jnp.float32), 0.099609375, 1.8984375).astype(jnp.bfloat16)
    return {"resid": resid, "pool_in": pool_in, "doc_ids": doc_ids, "w_group": w_group, "pool_scale": pool_scale, "w_branch": w_branch, "norm_gain": norm_gain, "route_ids": route_ids, "route_wts": route_wts, "w_exp_gate": w_exp_gate, "w_exp_up": w_exp_up, "w_exp_down": w_exp_down, "w_sh_gate": w_sh_gate, "w_sh_up": w_sh_up, "w_sh_down": w_sh_down, "final_gain": final_gain}


pool_windows = (2, 4, 8, 16, 16, 32, 64, 128)
alpha_mix = 8.0 ** 0.25
norm_eps = 1e-05

def layer_norm(values, scales):
    center = values - lax.optimization_barrier(jnp.mean(values, axis=-1, keepdims=True))
    spread = lax.optimization_barrier(jnp.mean(center * center, axis=-1, keepdims=True))
    return center * lax.rsqrt(spread + norm_eps) * scales.astype(jnp.float32)

def channel_windows(channel_count, group_width):
    groups = jnp.arange(channel_count, dtype=jnp.int32) // group_width
    window_table = jnp.asarray(pool_windows, dtype=jnp.int32)
    matches = groups[:, None] == jnp.arange(len(pool_windows), dtype=jnp.int32)[None, :]
    return lax.optimization_barrier(jnp.sum(jnp.where(matches, window_table[None, :], 0), axis=1)).astype(jnp.float32)

def swiglu_hidden(token_rows, gate_weight, up_weight):
    gate_vals = jnp.dot(token_rows, gate_weight, preferred_element_type=jnp.float32)
    up_vals = jnp.dot(token_rows, up_weight, preferred_element_type=jnp.float32)
    return (jax.nn.silu(gate_vals) * up_vals).astype(jnp.bfloat16)

def reference(resid, pool_in, doc_ids, w_group, pool_scale, w_branch, norm_gain, route_ids, route_wts, w_exp_gate, w_exp_up, w_exp_down, w_sh_gate, w_sh_up, w_sh_down, final_gain):
    values = pool_in.astype(jnp.float32)
    positions = jnp.arange(TOKENS, dtype=jnp.int32)
    change = jnp.concatenate([jnp.ones((1,), bool), doc_ids[1:] != doc_ids[:-1]])
    doc_start = lax.cummax(jnp.where(change, positions, 0), axis=0)
    since_start = (positions - doc_start).astype(jnp.float32)[:, None]
    cumulative = jnp.concatenate([jnp.zeros((1, P_SIZE), jnp.float32), jnp.cumsum(values, axis=0)], axis=0)
    current = cumulative[1:]
    running = current - cumulative[doc_start]
    doc_mean = running / (since_start + 1.0)
    widths = channel_windows(P_SIZE, GROUP_CH)[None, :]
    recent = running
    for window in sorted(set(pool_windows)):
        lagged = jnp.concatenate([jnp.zeros((window - 1, P_SIZE), jnp.float32), cumulative[:TOKENS + 1 - window]], axis=0)
        recent = jnp.where((widths == window) & (since_start >= window), current - lagged, recent)
    window_mean = recent / jnp.minimum(since_start + 1.0, widths)
    offset = (0.5 * (window_mean + doc_mean) - values).astype(jnp.bfloat16)
    mixed_rows = jnp.einsum('tgc,gcd->tgd', offset.reshape(TOKENS, GROUPS, GROUP_CH).astype(jnp.float32), w_group.astype(jnp.float32)).reshape(TOKENS, P_SIZE)
    mixed_rows = (mixed_rows * pool_scale.astype(jnp.float32)).astype(jnp.bfloat16)
    branch = jnp.dot(mixed_rows, w_branch, preferred_element_type=jnp.float32)
    normed = layer_norm(alpha_mix * resid.astype(jnp.float32) + branch, norm_gain).astype(jnp.bfloat16)
    flat_ids = route_ids.reshape(DEVICES, ROWS * TOPK)
    onehot = (flat_ids[:, :, None] == jnp.arange(EXPERTS, dtype=jnp.int32)[None, None, :]).astype(jnp.int32)
    slot_rank = lax.optimization_barrier(jnp.sum(jnp.cumsum(onehot, axis=1) * onehot, axis=2)) - 1
    block_index = jnp.arange(DEVICES, dtype=jnp.int32)[:, None]
    slot_index = (flat_ids * (DEVICES * CAP) + block_index * CAP + slot_rank).reshape(-1)
    assign_total = TOKENS * TOPK
    source = jnp.full((EXPERTS * DEVICES * CAP,), assign_total, jnp.int32)
    source = source.at[slot_index].set(jnp.arange(assign_total, dtype=jnp.int32)).reshape(EXPERTS, DEVICES * CAP)
    padded = jnp.concatenate([normed, jnp.zeros((1, D), jnp.bfloat16)], axis=0)
    weight_pad = jnp.concatenate([route_wts.reshape(-1), jnp.zeros((1,), jnp.float32)])

    def per_expert(accum, inputs):
        assign_ids, gate_weight, up_weight, down_weight = inputs
        token_ids = assign_ids // TOPK
        hidden = swiglu_hidden(padded[token_ids], gate_weight, up_weight)
        expert_out = jnp.dot(hidden, down_weight, preferred_element_type=jnp.float32).astype(jnp.bfloat16)
        scaled = weight_pad[assign_ids][:, None] * expert_out.astype(jnp.float32)
        return (accum.at[token_ids].add(scaled), None)
    routed, _ = lax.scan(per_expert, jnp.zeros((TOKENS + 1, D), jnp.float32), (source, w_exp_gate, w_exp_up, w_exp_down))
    routed = routed[:TOKENS]
    shared = jnp.dot(swiglu_hidden(normed, w_sh_gate, w_sh_up), w_sh_down, preferred_element_type=jnp.float32)
    return layer_norm(alpha_mix * normed.astype(jnp.float32) + routed + shared, final_gain).astype(jnp.bfloat16)
```

```python
import jax
import jax.numpy as jnp
import numpy as np
from jax import lax
from jax.sharding import Mesh, PartitionSpec as P

pool_windows = (2, 4, 8, 16, 16, 32, 64, 128)
alpha_mix = 8.0**0.25
norm_eps = 1e-05
SP = ("z", "x")
TP = ("y", "c")
PLANE = ("x", "y", "c")


def ring(value, axis, by):
    length = lax.axis_size(axis)
    return lax.ppermute(value, axis, [(i, (i + by) % length) for i in range(length)])


def shifted(value, axis, by):
    length = lax.axis_size(axis)
    pairs = [(i, i + by) for i in range(length) if 0 <= i + by < length]
    return lax.ppermute(value, axis, pairs)


def layer_norm(values, scales):
    center = values - jnp.mean(values, axis=-1, keepdims=True)
    spread = jnp.mean(center * center, axis=-1, keepdims=True)
    return center * lax.rsqrt(spread + norm_eps) * scales.astype(jnp.float32)


def swiglu_hidden(token_rows, gate_weight, up_weight):
    gate_vals = jnp.dot(token_rows, gate_weight, preferred_element_type=jnp.float32)
    up_vals = jnp.dot(token_rows, up_weight, preferred_element_type=jnp.float32)
    return (jax.nn.silu(gate_vals) * up_vals).astype(jnp.bfloat16)


def dot32(a, b):
    return jnp.dot(a, b, preferred_element_type=jnp.float32)


def gathered_rows(block):
    ny, nc = lax.axis_size("y"), lax.axis_size("c")
    y, c = lax.axis_index("y"), lax.axis_index("c")
    found = []
    part = block
    for i in range(ny):
        if i:
            part = ring(part, "y", 1)
        from_y = (y - i) % ny
        found.append((from_y * nc + c, part))
        other = part
        for j in range(1, nc):
            other = ring(other, "c", 1)
            found.append((from_y * nc + (c - j) % nc, other))
    return found


def pooled(pool_in, doc_ids, w_group, pool_scale):
    tok_count, local_width = pool_in.shape
    group_width = w_group.shape[1]
    group_count = local_width // group_width
    halo = max(pool_windows)
    tp_at = lax.axis_index(TP)
    sp_size, sp_at = lax.axis_size(SP), lax.axis_index(SP)
    before = shifted(pool_in[tok_count - halo :], SP, 1)
    last_doc = doc_ids[-1]
    trailing = (doc_ids == last_doc).astype(jnp.bfloat16)
    tail_sums = dot32(trailing[None, :], pool_in)
    tail_count = jnp.sum(trailing.astype(jnp.float32))
    lane = lax.broadcasted_iota(jnp.int32, (1, group_width), 1)
    info = jnp.where(lane == 0, last_doc.astype(jnp.float32), jnp.where(lane == 1, tail_count, 0.0))
    tail = jnp.concatenate([tail_sums, info], axis=1)
    tails = lax.all_to_all(
        jnp.broadcast_to(tail, (sp_size, tail.shape[1])), SP, split_axis=0, concat_axis=0, tiled=True
    )
    prev_doc = jnp.max(
        jnp.where(jnp.arange(sp_size) < sp_at, tails[:, local_width], -1.0)
    )
    joined = (jnp.arange(sp_size) < sp_at) & (tails[:, local_width] == prev_doc)
    prev = jnp.sum(jnp.where(joined[:, None], tails, 0.0), axis=0)
    prev_sums, prev_count = prev[:local_width], prev[local_width + 1]

    t = lax.broadcasted_iota(jnp.int32, (tok_count, tok_count), 0)
    s = lax.broadcasted_iota(jnp.int32, (tok_count, tok_count), 1)
    same = (doc_ids[:, None] == doc_ids[None, :]) & (s <= t)
    local_since = jnp.sum(same.astype(jnp.float32), axis=1) - 1.0
    running = dot32(same.astype(jnp.bfloat16), pool_in)
    table = jnp.asarray(pool_windows, dtype=jnp.int32)
    widths = [table[tp_at * group_count + g] for g in range(group_count)]
    recent = [
        dot32(
            (same & (s > t - widths[g])).astype(jnp.bfloat16),
            pool_in[:, g * group_width : (g + 1) * group_width],
        )
        for g in range(group_count)
    ]

    carried = doc_ids.astype(jnp.float32) == prev_doc
    since = (local_since + jnp.where(carried, prev_count, 0.0))[:, None]
    running = running + jnp.where(carried[:, None], prev_sums[None, :], 0.0)
    doc_mean = running / (since + 1.0)
    th = lax.broadcasted_iota(jnp.int32, (halo, halo), 0)
    sh = lax.broadcasted_iota(jnp.int32, (halo, halo), 1) - halo
    reach = (th - sh).astype(jnp.float32) <= since[:halo]
    local_groups = lax.dynamic_slice_in_dim(w_group, tp_at * group_count, group_count, 0)
    scale = lax.dynamic_slice_in_dim(pool_scale, tp_at * local_width, local_width, 0)
    scale = scale.astype(jnp.float32)[None, :]
    mixed = []
    for g in range(group_count):
        cols = slice(g * group_width, (g + 1) * group_width)
        early = dot32((reach & (sh > th - widths[g])).astype(jnp.bfloat16), before[:, cols])
        total = recent[g] + jnp.pad(early, ((0, tok_count - halo), (0, 0)))
        mean = total / jnp.minimum(since + 1.0, widths[g].astype(jnp.float32))
        offset = 0.5 * (mean + doc_mean[:, cols]) - pool_in[:, cols].astype(jnp.float32)
        rows = dot32(offset.astype(jnp.bfloat16), local_groups[g])
        mixed.append((rows * scale[:, cols]).astype(jnp.bfloat16))
    return jnp.concatenate(mixed, axis=1)


def slot_tables(packed, top, capacity):
    rows = packed.shape[1]
    per_plane = lax.axis_size(PLANE)
    first = lax.axis_index("z") * per_plane
    ids = packed[:top].astype(jnp.int32)
    experts = first + jnp.arange(per_plane, dtype=jnp.int32)
    hit = ids[:, None, :] == experts[None, :, None]
    member = jnp.any(hit, axis=0)
    weight = jnp.sum(jnp.where(hit, packed[top:][:, None, :], 0.0), axis=0)
    a = lax.broadcasted_iota(jnp.int32, (rows, rows), 0)
    b = lax.broadcasted_iota(jnp.int32, (rows, rows), 1)
    rank = dot32(member.astype(jnp.bfloat16), (a < b).astype(jnp.bfloat16)).astype(jnp.int32)
    slot = jnp.arange(capacity, dtype=jnp.int32)
    chosen = member[:, None, :] & (rank[:, None, :] == slot[None, :, None])
    slots = per_plane * capacity
    take = chosen.astype(jnp.bfloat16).reshape(slots, rows)
    spread = jnp.where(chosen, weight[:, None, :], 0.0).reshape(slots, rows)
    high = lax.reduce_precision(spread, 8, 7)
    give = jnp.concatenate([high, spread - high], axis=1).astype(jnp.bfloat16)
    return take, give


def local(
    resid,
    pool_in,
    doc_ids,
    w_group,
    pool_scale,
    w_branch,
    norm_gain,
    route_ids,
    route_wts,
    w_exp_gate,
    w_exp_up,
    w_exp_down,
    w_sh_gate,
    w_sh_up,
    w_sh_down,
    final_gain,
):
    row_count, model_width = resid.shape
    nz, per_plane, tp_size = lax.axis_size("z"), lax.axis_size(PLANE), lax.axis_size(TP)
    local_width = pool_in.shape[1]
    top = route_ids.shape[1]
    capacity = 2 * row_count * top // (nz * per_plane)
    packed = jnp.concatenate([route_ids.astype(jnp.float32), route_wts], axis=1).T
    tables = [
        slot_tables(ring(packed, "z", r) if r else packed, top, capacity) for r in range(nz)
    ]
    branch_rows = gathered_rows(w_branch)

    mixed = pooled(pool_in, doc_ids, w_group, pool_scale)
    parts = lax.all_to_all(
        mixed.reshape(tp_size, row_count, local_width), TP, split_axis=0, concat_axis=0, tiled=True
    )
    branch = 0.0
    for at, rows in branch_rows:
        branch = branch + dot32(lax.dynamic_index_in_dim(parts, at, 0, keepdims=False), rows)
    normed = layer_norm(alpha_mix * resid.astype(jnp.float32) + branch, norm_gain).astype(
        jnp.bfloat16
    )

    def across(value):
        value = value.reshape(per_plane, -1, model_width)
        value = lax.all_to_all(value, PLANE, split_axis=0, concat_axis=0, tiled=True)
        return value.reshape(-1, model_width)

    block = normed
    arrived = []
    for r in range(nz):
        if r:
            block = ring(block, "z", 1)
        arrived.append(across(dot32(tables[r][0], block).astype(jnp.bfloat16)))
    shared = dot32(swiglu_hidden(normed, w_sh_gate, w_sh_up), w_sh_down)

    routed = None
    for r in reversed(range(nz)):
        hidden = swiglu_hidden(arrived[r], w_exp_gate[0], w_exp_up[0])
        returned = across(dot32(hidden, w_exp_down[0]).astype(jnp.bfloat16))
        both = lax.dot_general(
            tables[r][1], returned, (((0,), (0,)), ((), ())), preferred_element_type=jnp.float32
        )
        partial = both[:row_count] + both[row_count:]
        routed = partial if routed is None else partial + routed.astype(jnp.float32)
        if r:
            routed = ring(routed.astype(jnp.bfloat16), "z", -1)
    return layer_norm(alpha_mix * normed.astype(jnp.float32) + routed + shared, final_gain).astype(
        jnp.bfloat16
    )


def axis_count(devices, at, whole):
    places = {getattr(d, "coords", (0, 0, 0))[at] for d in devices.flat}
    return len(places) if len(places) > 1 else whole


def solution(mesh):
    sp_size, tp_size = mesh.shape["sp"], mesh.shape["tp"]
    nz = axis_count(mesh.devices, 2, sp_size)
    ny = axis_count(mesh.devices, 1, tp_size)
    parted = Mesh(
        mesh.devices.reshape(nz, sp_size // nz, ny, tp_size // ny), ("z", "x", "y", "c")
    )
    every = SP + TP
    placed = (
        P(every, None),
        P(SP, TP),
        P(SP),
        P(),
        P(),
        P(TP, None),
        P(),
        P(every, None),
        P(every, None),
        P(every, None, None),
        P(every, None, None),
        P(every, None, None),
        P(),
        P(),
        P(),
        P(),
    )
    return jax.shard_map(
        local, mesh=parted, in_specs=placed, out_specs=P(every, None), check_vma=False
    )
```

```python
import jax
import jax.numpy as jnp
import numpy as np
from jax import lax
from jax.sharding import Mesh, PartitionSpec as P

pool_windows = (2, 4, 8, 16, 16, 32, 64, 128)
alpha_mix = 8.0**0.25
norm_eps = 1e-05
SP = ("z", "x")
TP = ("y", "c")
PLANE = ("x", "y", "c")


def ring(value, axis, by):
    length = lax.axis_size(axis)
    return lax.ppermute(value, axis, [(i, (i + by) % length) for i in range(length)])


def shifted(value, axis, by):
    length = lax.axis_size(axis)
    pairs = [(i, i + by) for i in range(length) if 0 <= i + by < length]
    return lax.ppermute(value, axis, pairs)


def layer_norm(values, scales):
    center = values - jnp.mean(values, axis=-1, keepdims=True)
    spread = jnp.mean(center * center, axis=-1, keepdims=True)
    return center * lax.rsqrt(spread + norm_eps) * scales.astype(jnp.float32)


def swiglu_hidden(token_rows, gate_weight, up_weight):
    gate_vals = jnp.dot(token_rows, gate_weight, preferred_element_type=jnp.float32)
    up_vals = jnp.dot(token_rows, up_weight, preferred_element_type=jnp.float32)
    return (jax.nn.silu(gate_vals) * up_vals).astype(jnp.bfloat16)


def dot32(a, b):
    return jnp.dot(a, b, preferred_element_type=jnp.float32)


def gathered_rows(block):
    ny, nc = lax.axis_size("y"), lax.axis_size("c")
    y, c = lax.axis_index("y"), lax.axis_index("c")
    found = []
    part = block
    for i in range(ny):
        if i:
            part = ring(part, "y", 1)
        from_y = jnp.where(y >= i, y - i, y - i + ny)
        found.append((from_y * nc + c, part))
        other = part
        for j in range(1, nc):
            other = ring(other, "c", 1)
            found.append((from_y * nc + jnp.where(c >= j, c - j, c - j + nc), other))
    return found


def after(value, other):
    return lax.optimization_barrier((value, other))[0]


def tail_of(pool_in, doc_ids, lanes):
    sp_size = lax.axis_size(SP)
    last_doc = doc_ids[-1]
    trailing = (doc_ids == last_doc).astype(jnp.bfloat16)
    tail_sums = dot32(trailing[None, :], pool_in)
    tail_count = jnp.sum(trailing.astype(jnp.float32))
    lane = lax.broadcasted_iota(jnp.int32, (1, lanes), 1)
    info = jnp.where(lane == 0, last_doc.astype(jnp.float32), jnp.where(lane == 1, tail_count, 0.0))
    tail = jnp.concatenate([tail_sums, info], axis=1)
    return jnp.broadcast_to(tail, (sp_size, tail.shape[1]))


def pooled(pool_in, doc_ids, w_group, pool_scale, tail, before):
    tok_count, local_width = pool_in.shape
    group_width = w_group.shape[1]
    group_count = local_width // group_width
    halo = max(pool_windows)
    tp_at = lax.axis_index(TP)
    sp_size, sp_at = lax.axis_size(SP), lax.axis_index(SP)
    tails = lax.all_to_all(tail, SP, split_axis=0, concat_axis=0, tiled=True)
    prev_doc = jnp.max(
        jnp.where(jnp.arange(sp_size) < sp_at, tails[:, local_width], -1.0)
    )
    joined = (jnp.arange(sp_size) < sp_at) & (tails[:, local_width] == prev_doc)
    prev = jnp.sum(jnp.where(joined[:, None], tails, 0.0), axis=0)
    prev_sums, prev_count = prev[:local_width], prev[local_width + 1]

    t = lax.broadcasted_iota(jnp.int32, (tok_count, tok_count), 0)
    s = lax.broadcasted_iota(jnp.int32, (tok_count, tok_count), 1)
    same = (doc_ids[:, None] == doc_ids[None, :]) & (s <= t)
    local_since = jnp.sum(same.astype(jnp.float32), axis=1) - 1.0
    running = dot32(same.astype(jnp.bfloat16), pool_in)
    widths = []
    for g in range(group_count):
        width = jnp.int32(pool_windows[g])
        for i in range(g, len(pool_windows), group_count):
            width = jnp.where(tp_at * group_count + g == i, pool_windows[i], width)
        widths.append(width)
    recent = [
        dot32(
            (same & (t - s < widths[g])).astype(jnp.bfloat16),
            pool_in[:, g * group_width : (g + 1) * group_width],
        )
        for g in range(group_count)
    ]

    carried = doc_ids.astype(jnp.float32) == prev_doc
    since = (local_since + jnp.where(carried, prev_count, 0.0))[:, None]
    running = running + jnp.where(carried[:, None], prev_sums[None, :], 0.0)
    doc_mean = running / (since + 1.0)
    th = lax.broadcasted_iota(jnp.int32, (halo, halo), 0)
    sh = lax.broadcasted_iota(jnp.int32, (halo, halo), 1) - halo
    reach = (th - sh).astype(jnp.float32) <= since[:halo]
    local_groups = lax.dynamic_slice_in_dim(w_group, tp_at * group_count, group_count, 0)
    scale = lax.dynamic_slice_in_dim(pool_scale, tp_at * local_width, local_width, 0)
    scale = scale.astype(jnp.float32)[None, :]
    mixed = []
    for g in range(group_count):
        cols = slice(g * group_width, (g + 1) * group_width)
        early = dot32((reach & (th - sh < widths[g])).astype(jnp.bfloat16), before[:, cols])
        total = recent[g] + jnp.pad(early, ((0, tok_count - halo), (0, 0)))
        mean = total / jnp.minimum(since + 1.0, widths[g].astype(jnp.float32))
        offset = 0.5 * (mean + doc_mean[:, cols]) - pool_in[:, cols].astype(jnp.float32)
        rows = dot32(offset.astype(jnp.bfloat16), local_groups[g])
        mixed.append((rows * scale[:, cols]).astype(jnp.bfloat16))
    return jnp.concatenate(mixed, axis=1)


def slot_tables(packed, top, capacity):
    rows = packed.shape[1]
    per_plane = lax.axis_size(PLANE)
    first = lax.axis_index("z") * per_plane
    ids = packed[:top].astype(jnp.int32)
    experts = first + jnp.arange(per_plane, dtype=jnp.int32)
    hit = ids[:, None, :] == experts[None, :, None]
    member = jnp.any(hit, axis=0)
    weight = jnp.sum(jnp.where(hit, packed[top:][:, None, :], 0.0), axis=0)
    a = lax.broadcasted_iota(jnp.int32, (rows, rows), 0)
    b = lax.broadcasted_iota(jnp.int32, (rows, rows), 1)
    rank = dot32(member.astype(jnp.bfloat16), (a < b).astype(jnp.bfloat16)).astype(jnp.int32)
    slot = jnp.arange(capacity, dtype=jnp.int32)
    chosen = member[:, None, :] & (rank[:, None, :] == slot[None, :, None])
    slots = per_plane * capacity
    take = chosen.astype(jnp.bfloat16).reshape(slots, rows)
    spread = jnp.where(chosen, weight[:, None, :], 0.0).reshape(slots, rows)
    high = lax.reduce_precision(spread, 8, 7)
    give = jnp.concatenate([high, spread - high], axis=1).astype(jnp.bfloat16)
    return take, give


def local(
    resid,
    pool_in,
    doc_ids,
    w_group,
    pool_scale,
    w_branch,
    norm_gain,
    route_ids,
    route_wts,
    w_exp_gate,
    w_exp_up,
    w_exp_down,
    w_sh_gate,
    w_sh_up,
    w_sh_down,
    final_gain,
):
    row_count, model_width = resid.shape
    nz, per_plane, tp_size = lax.axis_size("z"), lax.axis_size(PLANE), lax.axis_size(TP)
    local_width = pool_in.shape[1]
    top = route_ids.shape[1]
    capacity = 2 * row_count * top // (nz * per_plane)
    packed = jnp.concatenate([route_ids.astype(jnp.float32), route_wts], axis=1).T
    tail = tail_of(pool_in, doc_ids, w_group.shape[1])
    packed, w_branch = after(packed, tail), after(w_branch, tail)
    before = shifted(pool_in[pool_in.shape[0] - max(pool_windows) :], SP, 1)
    branch_rows = gathered_rows(w_branch)
    others = [ring(packed, "z", r) for r in range(1, nz)]

    mixed = pooled(pool_in, doc_ids, w_group, pool_scale, tail, before)
    first_table = slot_tables(after(packed, mixed), top, capacity)
    parts = lax.all_to_all(
        mixed.reshape(tp_size, row_count, local_width), TP, split_axis=0, concat_axis=0, tiled=True
    )
    branch = 0.0
    for at, rows in branch_rows:
        branch = branch + dot32(lax.dynamic_index_in_dim(parts, at, 0, keepdims=False), rows)
    normed = layer_norm(alpha_mix * resid.astype(jnp.float32) + branch, norm_gain).astype(
        jnp.bfloat16
    )

    def across(value):
        value = value.reshape(per_plane, -1, model_width)
        value = lax.all_to_all(value, PLANE, split_axis=0, concat_axis=0, tiled=True)
        return value.reshape(-1, model_width)

    rounds = [(r,) for r in range(nz)]
    tables = [first_table] + [
        slot_tables(after(other, normed), top, capacity) for other in others
    ]
    block = normed
    arrived = []
    for members in rounds:
        picked = []
        for r in members:
            if r:
                block = ring(block, "z", 1)
            rows = dot32(tables[r][0], block).astype(jnp.bfloat16)
            picked.append(rows.reshape(per_plane, capacity, model_width))
        arrived.append(across(jnp.concatenate(picked, axis=1)))
    shared = dot32(swiglu_hidden(normed, w_sh_gate, w_sh_up), w_sh_down)

    routed = None
    for members, rows in zip(reversed(rounds), reversed(arrived)):
        hidden = swiglu_hidden(rows, w_exp_gate[0], w_exp_up[0])
        returned = across(dot32(hidden, w_exp_down[0]).astype(jnp.bfloat16))
        returned = returned.reshape(per_plane, -1, model_width)
        for at in reversed(range(len(members))):
            r = members[at]
            mine = returned[:, at * capacity : (at + 1) * capacity].reshape(-1, model_width)
            both = lax.dot_general(
                tables[r][1], mine, (((0,), (0,)), ((), ())), preferred_element_type=jnp.float32
            )
            partial = both[:row_count] + both[row_count:]
            routed = partial if routed is None else partial + routed.astype(jnp.float32)
            if r:
                routed = ring(routed.astype(jnp.bfloat16), "z", -1)
    return layer_norm(alpha_mix * normed.astype(jnp.float32) + routed + shared, final_gain).astype(
        jnp.bfloat16
    )


def axis_count(devices, at, whole):
    places = {getattr(d, "coords", (0, 0, 0))[at] for d in devices.flat}
    return len(places) if len(places) > 1 else whole


def solution(mesh):
    sp_size, tp_size = mesh.shape["sp"], mesh.shape["tp"]
    nz = axis_count(mesh.devices, 2, sp_size)
    ny = axis_count(mesh.devices, 1, tp_size)
    parted = Mesh(
        mesh.devices.reshape(nz, sp_size // nz, ny, tp_size // ny), ("z", "x", "y", "c")
    )
    every = SP + TP
    placed = (
        P(every, None),
        P(SP, TP),
        P(SP),
        P(),
        P(),
        P(TP, None),
        P(),
        P(every, None),
        P(every, None),
        P(every, None, None),
        P(every, None, None),
        P(every, None, None),
        P(),
        P(),
        P(),
        P(),
    )
    return jax.shard_map(
        local, mesh=parted, in_specs=placed, out_specs=P(every, None), check_vma=False
    )
```
